128 devices in a mesh: fs: 16 (over z, y), tp: 8 (over x, core).
Axes of the slice: x: 4, y: 4, z: 4, core: 2. Of those that a mesh axis runs over, the one named last changes fastest.
Arguments:
- tokens: bfloat16 [16384, 2048], P(('fs', 'tp')), may hold values from -6 to 6
- routes: int32 [16384, 4], P(('fs', 'tp')), may hold values from 0 to 127, all different within a row; in each aligned block of 128 rows (0 to 127, 128 to 255, ...) at most 6 rows name the same one
- route_weight: float32 [16384, 4], P(('fs', 'tp')), may hold values from 0.1 to 1
- norm_gain: float32 [2048], P('fs'), may hold values from 0.5 to 4
- gate_weight: float32 [128, 2048, 512], P(None, 'fs', 'tp'), may hold values from -0.125 to 0.125
- up_weight: float32 [128, 2048, 512], P(None, 'fs', 'tp'), may hold values from -0.125 to 0.125
- down_weight: float32 [128, 512, 2048], P(None, 'fs', 'tp'), may hold values from -0.0625 to 0.0625
Outputs:
- gate_new: bfloat16 [128, 2048, 512], P(('fs', 'tp'))
- up_new: bfloat16 [128, 2048, 512], P(('fs', 'tp'))
- down_new: bfloat16 [128, 512, 2048], P(('fs', 'tp'))
- mixed: bfloat16 [16384, 2048], P(('fs', 'tp'))
The draws below stay inside these ranges and needn't reach their ends.
Inputs may be any that keep to these rules, and one draw needn't show every extreme that they name: `routes`: each row names 4 different experts, and every expert is named by some row; within the 128 rows of one device no expert is named by more than 6 rows, and in some blocks an expert is named by exactly 6 rows.
All inputs are finite; a program needn't handle non-finite values.
Results may differ from the reference program's by a relative error of at most 0.0084.
Values may be sent and summed in bfloat16 or wider, within the bound.
A program may use at most 128 MiB of HBM per device.

```python
import math
import jax
import jax.numpy as jnp
import numpy as np
from jax import lax

D = 2048
FF = 512
TOP_K = 4
TOK_DEV = 128
EXPERTS = 128
CAP = 6
TOKENS = 16384
N_FS = 16
N_TP = 8


def shard_levels(rng, shape, shards, least, largest):
    loudness, own = 1.0, jax.random.fold_in(rng, 6)
    for position, parts in shards:
        draws = jnp.exp(jax.random.uniform(jax.random.fold_in(own, position), (parts,), jnp.float32, least / len(shards), largest / len(shards)))
        loudness = loudness * jnp.repeat(draws, shape[position] // parts).reshape([-1 if axis == position else 1 for axis in range(len(shape))])
    return loudness


def shared_out(rng, own, number, rows, amount, top, reach, skew):
    ranking = jax.random.permutation(rng, amount)
    heavy_load, usual = portions_of(amount, rows * top, reach, skew, True), portions_of(amount, rows * top, reach, skew, False)
    places = jnp.arange(amount)

    def named(lengths, turn):
        used = int((lengths > 0).sum())
        fixed = max(1, used // 4)
        shifted = fixed + (places - fixed + turn * (used - fixed)) % max(1, amount - fixed)
        return jnp.zeros((amount,), jnp.int32).at[ranking[jnp.where(places < fixed, places, shifted)]].set(jnp.asarray(lengths, jnp.int32))

    lengths = jnp.where(number % 4 == 0, named(heavy_load, number // 4), named(usual, number - number // 4 - 1))
    mixed = jax.random.permutation(jax.random.fold_in(own, 3), amount)
    giver, sink = mixed[0:amount // 2 * 2:2], mixed[1:amount // 2 * 2:2]
    slack = jnp.minimum(lengths[giver] - 1, reach - lengths[sink]) // 2
    slack = jnp.where((giver == ranking[0]) | (sink == ranking[0]) | (lengths[sink] == 0), 0, jnp.maximum(slack, 0))
    shifted = jax.random.randint(jax.random.fold_in(own, 4), (amount // 2,), 0, 1 << 20) % (slack + 1)
    lengths = lengths.at[giver].add(-shifted).at[sink].add(shifted)
    members = jnp.searchsorted(jnp.cumsum(lengths), jnp.arange(rows * top), side="right").astype(jnp.int32)
    listing = members.reshape(top, rows).T
    listing = listing[jax.random.permutation(jax.random.fold_in(own, 1), rows)]
    turn = jax.random.randint(jax.random.fold_in(own, 2), (rows, 1), 0, top)
    return jnp.take_along_axis(listing, (jnp.arange(top)[None, :] + turn) % top, axis=1)


def portions_of(number_of, total, most, lean, full):
    weights = [(1 << 20) // math.isqrt(rank ** lean) + 1 for rank in range(1, number_of + 1)]
    largest = most if full else min(most, max(-(-total // number_of), total * weights[0] // sum(weights)))
    least = 1 if total - largest >= number_of - 1 else 0
    given, rest = [largest] + [least] * (number_of - 1), total - largest - least * (number_of - 1)
    while rest > 0:
        free = [i for i in range(1, number_of) if given[i] < largest] or [i for i in range(1, number_of) if given[i] < most]
        whole, remaining = sum([weights[i] for i in free]), rest
        for i in free:
            extra = min(most - given[i], max(1, remaining * weights[i] // whole), rest)
            given[i] = given[i] + extra
            rest = rest - extra
    return np.array(given)


def noise(stream_key, shape, deviation, most, split=(), held_as=jnp.bfloat16):
    values = jax.random.normal(stream_key, shape, jnp.float32) * deviation
    if len(split) > 0:
        values = shard_levels(stream_key, shape, split, -0.22, 0.18) * values
    return jnp.clip(values, min=-most, max=most).astype(held_as)


def setup_inputs(seed: int = 0) -> dict:
    streams_of = jax.random.split(jax.random.key(seed), 8)
    tokens = noise(streams_of[0], (TOKENS, D), 1.0, 6.0, ((0, 128),))
    routes_keys = jax.random.split(jax.random.fold_in(streams_of[1], 1), TOKENS // TOK_DEV)
    routes_turns = jax.random.permutation(jax.random.fold_in(streams_of[1], 3), TOKENS // TOK_DEV)
    routes = jax.vmap(lambda own, number: shared_out(jax.random.fold_in(streams_of[1], 2), own, number, TOK_DEV, EXPERTS, TOP_K, CAP, 1))(routes_keys, routes_turns).reshape((TOKENS, TOP_K))
    route_weight = jnp.clip(jnp.exp(math.log(1.0) - 2.3025851 * jax.random.uniform(streams_of[2], (TOKENS, TOP_K), jnp.float32) ** shard_levels(streams_of[2], (TOKENS, TOP_K), ((0, 128),), -0.2, 0.2)), 0.1, 1.0)
    norm_gain = jnp.clip(jnp.exp(math.log(4.0) - 2.0794415 * jax.random.uniform(streams_of[3], (D,), jnp.float32) ** shard_levels(streams_of[3], (D,), ((0, 16),), -0.2, 0.2)), 0.5, 4.0)
    gate_weight = noise(streams_of[4], (EXPERTS, D, FF), D ** -0.5, 0.125, ((1, 16), (2, 8)), jnp.float32)
    up_weight = noise(streams_of[5], (EXPERTS, D, FF), D ** -0.5, 0.125, ((1, 16), (2, 8)), jnp.float32)
    down_weight = noise(streams_of[6], (EXPERTS, FF, D), (16 * FF) ** -0.5, 0.0625, ((1, 16), (2, 8)), jnp.float32)
    return {"tokens": tokens, "routes": routes, "route_weight": route_weight, "norm_gain": norm_gain, "gate_weight": gate_weight, "up_weight": up_weight, "down_weight": down_weight}


norm_epsilon = 1e-06
clamp_limit = 7.0
sigmoid_slope = 1.702

def feed(inputs, gate_mat, up_mat, down_mat):
    gate_pre = jnp.dot(inputs, gate_mat, preferred_element_type=jnp.float32)
    up_pre = jnp.dot(inputs, up_mat, preferred_element_type=jnp.float32)
    gate_part = jnp.minimum(gate_pre, clamp_limit)
    linear_part = jnp.clip(up_pre, -clamp_limit, clamp_limit)
    activation = (gate_part * jax.nn.sigmoid(sigmoid_slope * gate_part) * (linear_part + 1.0)).astype(jnp.bfloat16)
    return jnp.dot(activation, down_mat, preferred_element_type=jnp.float32).astype(jnp.bfloat16)

def reference(tokens, routes, route_weight, norm_gain, gate_weight, up_weight, down_weight):
    gate_all = (gate_weight * norm_gain[None, :, None]).astype(jnp.bfloat16)
    up_all = (up_weight * norm_gain[None, :, None]).astype(jnp.bfloat16)
    down_all = down_weight.astype(jnp.bfloat16)
    values = tokens.astype(jnp.float32)
    squares = lax.optimization_barrier(jnp.mean(values * values, axis=1, keepdims=True))
    normed = (values * lax.rsqrt(squares + norm_epsilon)).astype(jnp.bfloat16)
    devices = N_FS * N_TP
    pair_experts = routes.reshape(devices, TOK_DEV * TOP_K)
    onehot = (pair_experts[:, :, None] == jnp.arange(EXPERTS, dtype=jnp.int32)[None, None, :]).astype(jnp.int32)
    earlier = jnp.cumsum(onehot, axis=1) - onehot
    rank = lax.optimization_barrier(jnp.sum(earlier * onehot, axis=2)).astype(jnp.int32)
    source_dev = jnp.arange(devices, dtype=jnp.int32)[:, None]
    column = (source_dev * CAP + rank).astype(jnp.int32)
    token_index = (source_dev * TOK_DEV + jnp.arange(TOK_DEV * TOP_K, dtype=jnp.int32)[None, :] // TOP_K).astype(jnp.int32)
    slot_table = jnp.full((EXPERTS, devices * CAP), TOKENS, jnp.int32).at[pair_experts, column].set(token_index)
    padded = jnp.concatenate([normed, jnp.zeros((1, D), jnp.bfloat16)], axis=0)

    def expert_rows(operands):
        rows_index, gate_mat, up_mat, down_mat = operands
        return feed(padded[rows_index], gate_mat, up_mat, down_mat)
    returned = lax.map(expert_rows, (slot_table, gate_all, up_all, down_all))
    picked = returned[pair_experts, column].reshape(TOKENS, TOP_K, D)
    mixed = lax.optimization_barrier(jnp.sum(picked.astype(jnp.float32) * route_weight[:, :, None], axis=1)).astype(jnp.bfloat16)
    return (gate_all, up_all, down_all, mixed)
```

```python
import jax
import jax.numpy as jnp
from jax import lax
from jax.experimental import pallas as pl
from jax.experimental.pallas import tpu as pltpu
from jax.sharding import PartitionSpec as P

MESH = pl.DeviceIdType.MESH
f32, bf16 = jnp.float32, jnp.bfloat16

norm_epsilon = 1e-06
clamp_limit = 7.0
sigmoid_slope = 1.702

N = 128
D = 2048
FF = 512
CAP = 6
PAD = 8
STRIDE = 101
LOADS = 8
ROWS = 256
GROUP = 16


def offset(k):
    kk = lax.rem(k * STRIDE, N)
    return kk // 32, lax.rem(kk // 8, 4), lax.rem(kk // 2, 4), lax.rem(kk, 2)


def kernel(
    tok, rt, rw, gain, g_in, u_in, d_in,
    g_out, u_out, d_out, m_out,
    g_stage, u_stage, d_stage, wsend, dsend, xsend, xrecv, gu, dn, osend, ret,
    act, gnew, selb, mixw, normed, total,
    load_sem, send_sem, recv_sem, ret_sem, out_sem,
):
    fs, tp = lax.axis_index("fs"), lax.axis_index("tp")
    z, y, x, c = fs // 4, lax.rem(fs, 4), tp // 2, lax.rem(tp, 2)
    me = fs * 8 + tp

    def ahead(k):
        dz, dy, dx, dc = offset(k)
        return (
            lax.rem(z + dz, 4) * 4 + lax.rem(y + dy, 4),
            lax.rem(x + dx, 4) * 2 + lax.rem(c + dc, 2),
        )

    def behind(k):
        dz, dy, dx, dc = offset(k)
        return (
            lax.rem(z + 4 - dz, 4) * 4 + lax.rem(y + 4 - dy, 4),
            lax.rem(x + 4 - dx, 4) * 2 + lax.rem(c + 2 - dc, 2),
        )

    per = N // LOADS

    def load(i, j):
        src, dst = ((g_in, g_stage), (u_in, u_stage), (d_in, d_stage))[j]
        part = pl.ds(i * per, per)
        return pltpu.make_async_copy(src.at[part], dst.at[part], load_sem.at[j, i])

    for i in range(LOADS):
        for j in range(3):
            load(i, j).start()

    barrier = pltpu.get_barrier_semaphore()

    def greet(k, carry):
        pl.semaphore_signal(barrier, inc=1, device_id=ahead(k), device_id_type=MESH)
        return carry

    lax.fori_loop(1, N, greet, 0)

    def iota(shape, dim):
        return lax.broadcasted_iota(jnp.int32, shape, dim)

    kk = (iota((N, N), 0) * STRIDE) & 127
    expert = (
        (((kk >> 5) + z) & 3) * 32
        + (((kk >> 3) + y) & 3) * 8
        + (((kk >> 1) + x) & 3) * 2
        + ((kk + c) & 1)
    )
    named = jnp.zeros((N, N), f32)
    weight = jnp.zeros((N, N), f32)
    for k in range(rt.shape[0]):
        hit = rt[k : k + 1, :] == expert
        named = jnp.where(hit, 1.0, named)
        weight = jnp.where(hit, rw[k : k + 1, :], weight)
    before = jnp.where(iota((N, N), 0) < iota((N, N), 1), 1.0, 0.0).astype(bf16)
    rank = jnp.dot(named.astype(bf16), before, preferred_element_type=f32)
    rank = jnp.where(named > 0.0, rank, -1.0)
    spread = jnp.where(iota((PAD * N, N), 0) // PAD == iota((PAD * N, N), 1), 1.0, 0.0)
    rows = jnp.dot(spread.astype(bf16), rank.astype(bf16), preferred_element_type=f32)
    place = (iota((PAD * N, N), 0) % PAD).astype(f32)
    selb[...] = jnp.where(rows == place, 1.0, 0.0).astype(bf16)

    spread_t = jnp.where(iota((N, PAD * N), 1) // PAD == iota((N, PAD * N), 0), 1.0, 0.0)
    spread_t = spread_t.astype(bf16)
    weight_t = weight.T
    high = weight_t.astype(bf16)
    low = (weight_t - high.astype(f32)).astype(bf16)
    lanes = jnp.dot(rank.T.astype(bf16), spread_t, preferred_element_type=f32)
    hit = lanes == (iota((N, PAD * N), 1) % PAD).astype(f32)
    for i, part in enumerate((high, low)):
        wide = jnp.dot(part, spread_t, preferred_element_type=f32)
        mixw[i * N : (i + 1) * N, :] = jnp.where(hit, wide, 0.0).astype(bf16)

    values = tok[...].astype(f32)
    squares = jnp.mean(values * values, axis=1, keepdims=True)
    normed[...] = (values * lax.rsqrt(squares + norm_epsilon)).astype(bf16)

    def pick(i, carry):
        part = selb[pl.ds(pl.multiple_of(i * N, N), N), :]
        picked = jnp.dot(part, normed[...], preferred_element_type=f32).astype(bf16)
        xsend[pl.ds(i * GROUP, GROUP)] = picked.reshape(GROUP, PAD, D)
        return carry

    lax.fori_loop(0, N // GROUP, pick, 0)

    scale = gain[...].reshape(1, 1, N)
    for i in range(LOADS):
        for j in range(3):
            load(i, j).wait()

        def round_one(e, carry):
            at = pl.ds(i * per + e * 2, 2)
            wsend[at, 0] = (g_stage[at] * scale).astype(bf16)
            wsend[at, 1] = (u_stage[at] * scale).astype(bf16)
            dsend[at] = d_stage[at].astype(bf16)
            return carry

        lax.fori_loop(0, per // 2, round_one, 0)

    pl.semaphore_wait(barrier, N - 1)

    my_rows = pl.ds(pl.multiple_of(tp * 64, 64), 64)
    my_cols = pl.ds(pl.multiple_of(fs * 128, 128), 128)
    down_rows = pl.ds(pl.multiple_of(fs * 32, 32), 32)
    down_cols = pl.ds(pl.multiple_of(tp * 256, 256), 256)

    def remote(src, dst, i, to):
        return pltpu.make_async_remote_copy(
            src_ref=src, dst_ref=dst, send_sem=send_sem.at[i], recv_sem=recv_sem.at[i],
            device_id=to, device_id_type=MESH,
        )

    def send_first(k, carry):
        to = ahead(k)
        t = to[0] * 8 + to[1]
        remote(xsend.at[k, pl.ds(0, CAP)], xrecv.at[k, pl.ds(0, CAP)], 0, to).start()
        remote(wsend.at[t], gu.at[:, my_rows, my_cols], 1, to).start()
        return carry

    def send_second(k, carry):
        to = ahead(k)
        t = to[0] * 8 + to[1]
        remote(dsend.at[t], dn.at[down_rows, down_cols], 2, to).start()
        return carry

    lax.fori_loop(1, N, send_first, 0)
    lax.fori_loop(1, N, send_second, 0)

    xrecv[0] = xsend[0]
    gu[:, my_rows, my_cols] = wsend[me]
    dn[down_rows, down_cols] = dsend[me]

    other = (fs, tp + 1 - 2 * c)
    others = pl.ds(0, N - 1)
    all_rows = remote(xsend.at[others, pl.ds(0, CAP)], xrecv.at[others, pl.ds(0, CAP)], 0, other)
    all_tiles = remote(wsend.at[others], wsend.at[others], 1, other)
    all_down = remote(dsend.at[others], dsend.at[others], 2, other)

    all_rows.wait_recv()
    all_tiles.wait_recv()

    wide = (((1,), (1,)), ((), ()))

    def first(j, carry):
        block = xrecv[pl.ds(j * (ROWS // PAD), ROWS // PAD)].reshape(ROWS, D)
        gate_pre = lax.dot_general(block, gu[0], wide, preferred_element_type=f32)
        up_pre = lax.dot_general(block, gu[1], wide, preferred_element_type=f32)
        gate_part = jnp.minimum(gate_pre, clamp_limit)
        linear_part = jnp.clip(up_pre, -clamp_limit, clamp_limit)
        result = gate_part * jax.nn.sigmoid(sigmoid_slope * gate_part) * (linear_part + 1.0)
        act[pl.ds(pl.multiple_of(j * ROWS, ROWS), ROWS), :] = result.astype(bf16)
        return carry

    lax.fori_loop(0, PAD * N // ROWS, first, 0)

    all_down.wait_recv()

    def back(k, carry):
        pltpu.make_async_remote_copy(
            src_ref=osend.at[k, pl.ds(0, CAP)], dst_ref=ret.at[k, pl.ds(0, CAP)],
            send_sem=send_sem.at[3], recv_sem=ret_sem.at[k // GROUP],
            device_id=behind(k), device_id_type=MESH,
        ).start()
        return carry

    def second(j, carry):
        part = act[pl.ds(pl.multiple_of(j * N, N), N), :]
        result = jnp.dot(part, dn[...], preferred_element_type=f32).astype(bf16)
        osend[pl.ds(j * GROUP, GROUP)] = result.reshape(GROUP, PAD, D)

        @pl.when(j > 0)
        def _():
            lax.fori_loop(lax.max((j - 1) * GROUP, 1), j * GROUP, back, 0)

        return carry

    steps = N // GROUP
    lax.fori_loop(0, steps, second, 0)
    ret[0] = osend[0]
    lax.fori_loop(N - GROUP, N, back, 0)

    for j in range(2):
        def turn(b, carry):
            at = pl.ds(pl.multiple_of(b * 128, 128), 128)
            gnew[j, at, :] = gu[j, :, at].astype(f32).T.astype(bf16)
            return carry

        lax.fori_loop(0, D // 128, turn, 0)

    total[...] = jnp.zeros_like(total)
    outs = (
        pltpu.make_async_copy(gnew.at[0], g_out, out_sem.at[0]),
        pltpu.make_async_copy(gnew.at[1], u_out, out_sem.at[1]),
        pltpu.make_async_copy(dn, d_out, out_sem.at[2]),
    )
    for copy in outs:
        copy.start()

    for j in range(steps):
        count = GROUP - 1 if j == 0 else GROUP
        part = pl.ds(j * GROUP, count)
        pltpu.make_async_remote_copy(
            src_ref=osend.at[part, pl.ds(0, CAP)], dst_ref=ret.at[part, pl.ds(0, CAP)],
            send_sem=send_sem.at[3], recv_sem=ret_sem.at[j],
            device_id=other, device_id_type=MESH,
        ).wait_recv()
        block = ret[j * GROUP : (j + 1) * GROUP]
        block = jnp.where(iota(block.shape, 1) < CAP, block, jnp.zeros_like(block))
        both = jnp.dot(
            mixw[:, j * N : (j + 1) * N], block.reshape(N, D), preferred_element_type=f32
        )
        total[...] += both[:N] + both[N:]
    m_out[...] = total[...].astype(bf16)

    for copy in outs:
        copy.wait()
    all_rows.wait_send()
    all_tiles.wait_send()
    all_down.wait_send()
    remote(osend.at[others, pl.ds(0, CAP)], ret.at[others, pl.ds(0, CAP)], 3, other).wait_send()


def shards(tokens, routes, route_weight, norm_gain, gate_weight, up_weight, down_weight):
    vmem = pl.BlockSpec(memory_space=pltpu.VMEM)
    anywhere = pl.BlockSpec(memory_space=pl.ANY)
    gate_new, up_new, down_new, mixed = pl.pallas_call(
        kernel,
        out_shape=(
            jax.ShapeDtypeStruct((D, FF), bf16),
            jax.ShapeDtypeStruct((D, FF), bf16),
            jax.ShapeDtypeStruct((FF, D), bf16),
            jax.ShapeDtypeStruct((N, D), bf16),
        ),
        in_specs=[vmem, vmem, vmem, vmem, anywhere, anywhere, anywhere],
        out_specs=(anywhere, anywhere, anywhere, vmem),
        scratch_shapes=[
            pltpu.VMEM((N, 64, 128), f32),
            pltpu.VMEM((N, 64, 128), f32),
            pltpu.VMEM((N, 32, 256), f32),
            pltpu.VMEM((N, 2, 64, 128), bf16),
            pltpu.VMEM((N, 32, 256), bf16),
            pltpu.VMEM((N, PAD, D), bf16),
            pltpu.VMEM((N, PAD, D), bf16),
            pltpu.VMEM((2, FF, D), bf16),
            pltpu.VMEM((FF, D), bf16),
            pltpu.VMEM((N, PAD, D), bf16),
            pltpu.VMEM((N, PAD, D), bf16),
            pltpu.VMEM((PAD * N, FF), bf16),
            pltpu.VMEM((2, D, FF), bf16),
            pltpu.VMEM((PAD * N, N), bf16),
            pltpu.VMEM((2 * N, PAD * N), bf16),
            pltpu.VMEM((N, D), bf16),
            pltpu.VMEM((N, D), f32),
            pltpu.SemaphoreType.DMA((3, LOADS)),
            pltpu.SemaphoreType.DMA((4,)),
            pltpu.SemaphoreType.DMA((3,)),
            pltpu.SemaphoreType.DMA((N // GROUP,)),
            pltpu.SemaphoreType.DMA((3,)),
        ],
        compiler_params=pltpu.CompilerParams(
            collective_id=0, has_side_effects=True, vmem_limit_bytes=67043328
        ),
    )(
        tokens,
        routes.T,
        route_weight.T,
        norm_gain.reshape(1, N),
        jnp.swapaxes(gate_weight, 1, 2),
        jnp.swapaxes(up_weight, 1, 2),
        down_weight,
    )
    return gate_new[None], up_new[None], down_new[None], mixed


def solution(mesh):
    placed = (
        P(("fs", "tp"), None),
        P(("fs", "tp"), None),
        P(("fs", "tp"), None),
        P("fs"),
        P(None, "fs", "tp"),
        P(None, "fs", "tp"),
        P(None, "fs", "tp"),
    )
    return jax.shard_map(
        shards,
        mesh=mesh,
        in_specs=placed,
        out_specs=(
            P(("fs", "tp"), None, None),
            P(("fs", "tp"), None, None),
            P(("fs", "tp"), None, None),
            P(("fs", "tp"), None),
        ),
        check_vma=False,
    )
```

```python
import jax
import jax.numpy as jnp
from jax import lax
from jax.experimental import pallas as pl
from jax.experimental.pallas import tpu as pltpu
from jax.sharding import PartitionSpec as P

MESH = pl.DeviceIdType.MESH
f32, bf16 = jnp.float32, jnp.bfloat16

norm_epsilon = 1e-06
clamp_limit = 7.0
sigmoid_slope = 1.702

N = 128
D = 2048
FF = 512
CAP = 6
PAD = 8
STRIDE = 59
LOADS = 8
ROWS = 256
HALF = 64
GROUP = 16


def offset(k):
    kk = lax.rem(k * STRIDE, N)
    return kk // 32, lax.rem(kk // 8, 4), lax.rem(kk // 2, 4), lax.rem(kk, 2)


def kernel(
    tok, rt, rw, gain, g_in, u_in, d_in,
    gate_new, up_new, dn, m_out,
    g_stage, u_stage, d_stage, wsend, dsend, xsend, xrecv, gu, osend, ret,
    act, selb, mixw, normed, total,
    load_sem, send_sem, recv_sem, ret_sem,
):
    fs, tp = lax.axis_index("fs"), lax.axis_index("tp")
    z, y, x, c = fs // 4, lax.rem(fs, 4), tp // 2, lax.rem(tp, 2)
    me = fs * 8 + tp

    def ahead(k):
        dz, dy, dx, dc = offset(k)
        return (
            lax.rem(z + dz, 4) * 4 + lax.rem(y + dy, 4),
            lax.rem(x + dx, 4) * 2 + lax.rem(c + dc, 2),
        )

    def behind(k):
        dz, dy, dx, dc = offset(k)
        return (
            lax.rem(z + 4 - dz, 4) * 4 + lax.rem(y + 4 - dy, 4),
            lax.rem(x + 4 - dx, 4) * 2 + lax.rem(c + 2 - dc, 2),
        )

    per = N // LOADS

    def load(i, j):
        src, dst = ((g_in, g_stage), (u_in, u_stage), (d_in, d_stage))[j]
        part = pl.ds(i * per, per)
        return pltpu.make_async_copy(src.at[part], dst.at[part], load_sem.at[j, i])

    for i in range(LOADS):
        for j in range(3):
            load(i, j).start()

    barrier = pltpu.get_barrier_semaphore()

    def greet(k, carry):
        pl.semaphore_signal(barrier, inc=1, device_id=ahead(k), device_id_type=MESH)
        return carry

    lax.fori_loop(1, N, greet, 0)

    def iota(shape, dim):
        return lax.broadcasted_iota(jnp.int32, shape, dim)

    kk = (iota((N, N), 0) * STRIDE) & 127
    expert = (
        (((kk >> 5) + z) & 3) * 32
        + (((kk >> 3) + y) & 3) * 8
        + (((kk >> 1) + x) & 3) * 2
        + ((kk + c) & 1)
    )
    named = jnp.zeros((N, N), f32)
    weight = jnp.zeros((N, N), f32)
    for k in range(rt.shape[0]):
        hit = rt[k : k + 1, :] == expert
        named = jnp.where(hit, 1.0, named)
        weight = jnp.where(hit, rw[k : k + 1, :], weight)
    before = jnp.where(iota((N, N), 0) < iota((N, N), 1), 1.0, 0.0).astype(bf16)
    rank = jnp.dot(named.astype(bf16), before, preferred_element_type=f32)
    rank = jnp.where(named > 0.0, rank, -1.0)
    spread = jnp.where(iota((PAD * N, N), 0) // PAD == iota((PAD * N, N), 1), 1.0, 0.0)
    rows = jnp.dot(spread.astype(bf16), rank.astype(bf16), preferred_element_type=f32)
    place = (iota((PAD * N, N), 0) % PAD).astype(f32)
    selb[...] = jnp.where(rows == place, 1.0, 0.0).astype(bf16)

    values = tok[...].astype(f32)
    squares = jnp.mean(values * values, axis=1, keepdims=True)
    normed[...] = (values * lax.rsqrt(squares + norm_epsilon)).astype(bf16)

    def pick(i, carry):
        part = selb[pl.ds(pl.multiple_of(i * N, N), N), :]
        picked = jnp.dot(part, normed[...], preferred_element_type=f32).astype(bf16)
        xsend[pl.ds(i * GROUP, GROUP)] = picked.reshape(GROUP, PAD, D)
        return carry

    lax.fori_loop(0, N // GROUP, pick, 0)

    pl.semaphore_wait(barrier, N - 1)

    my_rows = pl.ds(pl.multiple_of(tp * 64, 64), 64)
    my_cols = pl.ds(pl.multiple_of(fs * 128, 128), 128)
    down_rows = pl.ds(pl.multiple_of(fs * 32, 32), 32)
    down_cols = pl.ds(pl.multiple_of(tp * 256, 256), 256)

    def remote(src, dst, i, to):
        return pltpu.make_async_remote_copy(
            src_ref=src, dst_ref=dst, send_sem=send_sem.at[i], recv_sem=recv_sem.at[i],
            device_id=to, device_id_type=MESH,
        )

    def send_rows(half):
        def send(k, carry):
            part = pl.ds(0, CAP)
            remote(xsend.at[k, part], xrecv.at[k, part], half, ahead(k)).start()
            return carry

        return send

    def send_tiles(k, carry):
        to = ahead(k)
        remote(wsend.at[to[0] * 8 + to[1]], gu.at[:, my_rows, my_cols], 2, to).start()
        return carry

    def send_down(k, carry):
        to = ahead(k)
        remote(dsend.at[to[0] * 8 + to[1]], dn.at[down_rows, down_cols], 3, to).start()
        return carry

    lax.fori_loop(1, HALF, send_rows(0), 0)

    scale = gain[...].reshape(1, 1, N)
    for i in range(LOADS):
        for j in range(3):
            load(i, j).wait()

        def round_one(e, carry):
            at = pl.ds(i * per + e * 2, 2)
            wsend[at, 0] = (g_stage[at] * scale).astype(bf16)
            wsend[at, 1] = (u_stage[at] * scale).astype(bf16)
            dsend[at] = d_stage[at].astype(bf16)
            return carry

        lax.fori_loop(0, per // 2, round_one, 0)

    lax.fori_loop(1, N, send_tiles, 0)
    lax.fori_loop(1, N, send_down, 0)
    lax.fori_loop(HALF, N, send_rows(1), 0)

    xrecv[0] = xsend[0]
    gu[:, my_rows, my_cols] = wsend[me]
    dn[down_rows, down_cols] = dsend[me]

    spread_t = jnp.where(iota((N, PAD * N), 1) // PAD == iota((N, PAD * N), 0), 1.0, 0.0)
    spread_t = spread_t.astype(bf16)
    weight_t = weight.T
    high = weight_t.astype(bf16)
    low = (weight_t - high.astype(f32)).astype(bf16)
    lanes = jnp.dot(rank.T.astype(bf16), spread_t, preferred_element_type=f32)
    hit = lanes == (iota((N, PAD * N), 1) % PAD).astype(f32)
    for i, part in enumerate((high, low)):
        wide = jnp.dot(part, spread_t, preferred_element_type=f32)
        mixw[i * N : (i + 1) * N, :] = jnp.where(hit, wide, 0.0).astype(bf16)

    other = (fs, tp + 1 - 2 * c)
    others = pl.ds(0, N - 1)
    early, late = pl.ds(0, HALF - 1), pl.ds(0, N - HALF)
    early_rows = remote(xsend.at[early, pl.ds(0, CAP)], xrecv.at[early, pl.ds(0, CAP)], 0, other)
    late_rows = remote(xsend.at[late, pl.ds(0, CAP)], xrecv.at[late, pl.ds(0, CAP)], 1, other)
    all_tiles = remote(wsend.at[others], wsend.at[others], 2, other)
    all_down = remote(dsend.at[others], dsend.at[others], 3, other)

    wide = (((1,), (1,)), ((), ()))

    def first(j, carry):
        block = xrecv[pl.ds(j * (ROWS // PAD), ROWS // PAD)].reshape(ROWS, D)
        gate_pre = lax.dot_general(block, gu[0], wide, preferred_element_type=f32)
        up_pre = lax.dot_general(block, gu[1], wide, preferred_element_type=f32)
        gate_part = jnp.minimum(gate_pre, clamp_limit)
        linear_part = jnp.clip(up_pre, -clamp_limit, clamp_limit)
        result = gate_part * jax.nn.sigmoid(sigmoid_slope * gate_part) * (linear_part + 1.0)
        act[pl.ds(pl.multiple_of(j * ROWS, ROWS), ROWS), :] = result.astype(bf16)
        return carry

    def back(k, carry):
        pltpu.make_async_remote_copy(
            src_ref=osend.at[k, pl.ds(0, CAP)], dst_ref=ret.at[k, pl.ds(0, CAP)],
            send_sem=send_sem.at[4], recv_sem=ret_sem.at[k // GROUP],
            device_id=behind(k), device_id_type=MESH,
        ).start()
        return carry

    def second(begin):
        def body(j, carry):
            part = act[pl.ds(pl.multiple_of(j * N, N), N), :]
            result = jnp.dot(part, dn[...], preferred_element_type=f32).astype(bf16)
            osend[pl.ds(j * GROUP, GROUP)] = result.reshape(GROUP, PAD, D)

            @pl.when(j > begin)
            def _():
                lax.fori_loop(lax.max((j - 1) * GROUP, 1), j * GROUP, back, 0)

            return carry

        return body

    early_rows.wait_recv()
    all_tiles.wait_recv()
    lax.fori_loop(0, PAD * HALF // ROWS, first, 0)
    all_down.wait_recv()
    lax.fori_loop(0, HALF // GROUP, second(0), 0)
    ret[0] = osend[0]
    lax.fori_loop(HALF - GROUP, HALF, back, 0)

    late_rows.wait_recv()
    lax.fori_loop(PAD * HALF // ROWS, PAD * N // ROWS, first, 0)
    lax.fori_loop(HALF // GROUP, N // GROUP, second(HALF // GROUP), 0)
    lax.fori_loop(N - GROUP, N, back, 0)

    for j, new in enumerate((gate_new, up_new)):
        def turn(b, carry):
            at = pl.ds(pl.multiple_of(b * 128, 128), 128)
            new[at, :] = gu[j, :, at].astype(f32).T.astype(bf16)
            return carry

        lax.fori_loop(0, D // 128, turn, 0)

    total[...] = jnp.zeros_like(total)
    for j in range(N // GROUP):
        count = GROUP - 1 if j == 0 else GROUP
        part = pl.ds(j * GROUP, count)
        pltpu.make_async_remote_copy(
            src_ref=osend.at[part, pl.ds(0, CAP)], dst_ref=ret.at[part, pl.ds(0, CAP)],
            send_sem=send_sem.at[4], recv_sem=ret_sem.at[j],
            device_id=other, device_id_type=MESH,
        ).wait_recv()
        block = ret[j * GROUP : (j + 1) * GROUP]
        block = jnp.where(iota(block.shape, 1) < CAP, block, jnp.zeros_like(block))
        both = jnp.dot(
            mixw[:, j * N : (j + 1) * N], block.reshape(N, D), preferred_element_type=f32
        )
        total[...] += both[:N] + both[N:]
    m_out[...] = total[...].astype(bf16)

    early_rows.wait_send()
    late_rows.wait_send()
    all_tiles.wait_send()
    all_down.wait_send()
    pltpu.make_async_remote_copy(
        src_ref=osend.at[others, pl.ds(0, CAP)], dst_ref=ret.at[others, pl.ds(0, CAP)],
        send_sem=send_sem.at[4], recv_sem=ret_sem.at[0], device_id=other, device_id_type=MESH,
    ).wait_send()


def shards(tokens, routes, route_weight, norm_gain, gate_weight, up_weight, down_weight):
    vmem = pl.BlockSpec(memory_space=pltpu.VMEM)
    anywhere = pl.BlockSpec(memory_space=pl.ANY)
    gate_new, up_new, down_new, mixed = pl.pallas_call(
        kernel,
        out_shape=(
            pltpu.VMEM((D, FF), bf16),
            pltpu.VMEM((D, FF), bf16),
            pltpu.VMEM((FF, D), bf16),
            pltpu.VMEM((N, D), bf16),
        ),
        in_specs=[vmem, vmem, vmem, vmem, anywhere, anywhere, anywhere],
        out_specs=(vmem, vmem, vmem, vmem),
        scratch_shapes=[
            pltpu.VMEM((N, 64, 128), f32),
            pltpu.VMEM((N, 64, 128), f32),
            pltpu.VMEM((N, 32, 256), f32),
            pltpu.VMEM((N, 2, 64, 128), bf16),
            pltpu.VMEM((N, 32, 256), bf16),
            pltpu.VMEM((N, PAD, D), bf16),
            pltpu.VMEM((N, PAD, D), bf16),
            pltpu.VMEM((2, FF, D), bf16),
            pltpu.VMEM((N, PAD, D), bf16),
            pltpu.VMEM((N, PAD, D), bf16),
            pltpu.VMEM((PAD * N, FF), bf16),
            pltpu.VMEM((PAD * N, N), bf16),
            pltpu.VMEM((2 * N, PAD * N), bf16),
            pltpu.VMEM((N, D), bf16),
            pltpu.VMEM((N, D), f32),
            pltpu.SemaphoreType.DMA((3, LOADS)),
            pltpu.SemaphoreType.DMA((5,)),
            pltpu.SemaphoreType.DMA((4,)),
            pltpu.SemaphoreType.DMA((N // GROUP,)),
        ],
        compiler_params=pltpu.CompilerParams(
            collective_id=0, has_side_effects=True, vmem_limit_bytes=55 * 2**20
        ),
    )(
        tokens,
        routes.T,
        route_weight.T,
        norm_gain.reshape(1, N),
        jnp.swapaxes(gate_weight, 1, 2),
        jnp.swapaxes(up_weight, 1, 2),
        down_weight,
    )
    return gate_new[None], up_new[None], down_new[None], mixed


def solution(mesh):
    placed = (
        P(("fs", "tp"), None),
        P(("fs", "tp"), None),
        P(("fs", "tp"), None),
        P("fs"),
        P(None, "fs", "tp"),
        P(None, "fs", "tp"),
        P(None, "fs", "tp"),
    )
    return jax.shard_map(
        shards,
        mesh=mesh,
        in_specs=placed,
        out_specs=(
            P(("fs", "tp"), None, None),
            P(("fs", "tp"), None, None),
            P(("fs", "tp"), None, None),
            P(("fs", "tp"), None),
        ),
        check_vma=False,
    )
```

```python
import jax
import jax.numpy as jnp
from jax import lax
from jax.experimental import pallas as pl
from jax.experimental.pallas import tpu as pltpu
from jax.sharding import PartitionSpec as P

MESH = pl.DeviceIdType.MESH
f32, bf16 = jnp.float32, jnp.bfloat16

norm_epsilon = 1e-06
clamp_limit = 7.0
sigmoid_slope = 1.702

N = 128
D = 2048
FF = 512
CAP = 6
PAD = 8
STRIDE = 59
LOADS = 8
ROWS = 256
HALF = 64
GROUP = 16


def offset(k):
    kk = lax.rem(k * STRIDE, N)
    return kk // 32, lax.rem(kk // 8, 4), lax.rem(kk // 2, 4), lax.rem(kk, 2)


def kernel(
    tok, rt, rw, gain, g_in, u_in, d_in,
    gate_new, up_new, dn, m_out,
    g_stage, u_stage, d_stage, wsend, dsend, xsend, xrecv, gu, osend, ret,
    act, selb, mixw, normed, total,
    load_sem, send_sem, recv_sem, ret_sem,
):
    fs, tp = lax.axis_index("fs"), lax.axis_index("tp")
    z, y, x, c = fs // 4, lax.rem(fs, 4), tp // 2, lax.rem(tp, 2)
    me = fs * 8 + tp

    def ahead(k):
        dz, dy, dx, dc = offset(k)
        return (
            lax.rem(z + dz, 4) * 4 + lax.rem(y + dy, 4),
            lax.rem(x + dx, 4) * 2 + lax.rem(c + dc, 2),
        )

    def behind(k):
        dz, dy, dx, dc = offset(k)
        return (
            lax.rem(z + 4 - dz, 4) * 4 + lax.rem(y + 4 - dy, 4),
            lax.rem(x + 4 - dx, 4) * 2 + lax.rem(c + 2 - dc, 2),
        )

    per = N // LOADS

    def load(i, j):
        src, dst = ((g_in, g_stage), (u_in, u_stage), (d_in, d_stage))[j]
        part = pl.ds(i * per, per)
        return pltpu.make_async_copy(src.at[part], dst.at[part], load_sem.at[j, i])

    for i in range(LOADS):
        for j in range(3):
            load(i, j).start()

    barrier = pltpu.get_barrier_semaphore()

    def greet(k, carry):
        pl.semaphore_signal(barrier, inc=1, device_id=ahead(k), device_id_type=MESH)
        return carry

    lax.fori_loop(1, N, greet, 0)

    def iota(shape, dim):
        return lax.broadcasted_iota(jnp.int32, shape, dim)

    kk = (iota((N, N), 0) * STRIDE) & 127
    expert = (
        (((kk >> 5) + z) & 3) * 32
        + (((kk >> 3) + y) & 3) * 8
        + (((kk >> 1) + x) & 3) * 2
        + ((kk + c) & 1)
    )
    named = jnp.zeros((N, N), f32)
    weight = jnp.zeros((N, N), f32)
    for k in range(rt.shape[0]):
        hit = rt[k : k + 1, :] == expert
        named = jnp.where(hit, 1.0, named)
        weight = jnp.where(hit, rw[k : k + 1, :], weight)
    before = jnp.where(iota((N, N), 0) < iota((N, N), 1), 1.0, 0.0).astype(bf16)
    rank = jnp.dot(named.astype(bf16), before, preferred_element_type=f32)
    rank = jnp.where(named > 0.0, rank, -1.0)
    spread = jnp.where(iota((PAD * N, N), 0) // PAD == iota((PAD * N, N), 1), 1.0, 0.0)
    rows = jnp.dot(spread.astype(bf16), rank.astype(bf16), preferred_element_type=f32)
    place = (iota((PAD * N, N), 0) % PAD).astype(f32)
    selb[...] = jnp.where(rows == place, 1.0, 0.0).astype(bf16)

    values = tok[...].astype(f32)
    squares = jnp.mean(values * values, axis=1, keepdims=True)
    normed[...] = (values * lax.rsqrt(squares + norm_epsilon)).astype(bf16)

    def pick(i, carry):
        part = selb[pl.ds(pl.multiple_of(i * N, N), N), :]
        picked = jnp.dot(part, normed[...], preferred_element_type=f32).astype(bf16)
        xsend[pl.ds(i * GROUP, GROUP)] = picked.reshape(GROUP, PAD, D)
        return carry

    lax.fori_loop(0, N // GROUP, pick, 0)

    pl.semaphore_wait(barrier, N - 1)

    my_rows = pl.ds(pl.multiple_of(tp * 64, 64), 64)
    my_cols = pl.ds(pl.multiple_of(fs * 128, 128), 128)
    down_rows = pl.ds(pl.multiple_of(fs * 32, 32), 32)
    down_cols = pl.ds(pl.multiple_of(tp * 256, 256), 256)

    def remote(src, dst, i, to):
        return pltpu.make_async_remote_copy(
            src_ref=src, dst_ref=dst, send_sem=send_sem.at[i], recv_sem=recv_sem.at[i],
            device_id=to, device_id_type=MESH,
        )

    def send_rows(half):
        def send(k, carry):
            part = pl.ds(0, CAP)
            remote(xsend.at[k, part], xrecv.at[k, part], half, ahead(k)).start()
            return carry

        return send

    def send_tiles(k, carry):
        to = ahead(k)
        remote(wsend.at[to[0] * 8 + to[1]], gu.at[:, my_rows, my_cols], 2, to).start()
        return carry

    def send_down(k, carry):
        to = ahead(k)
        remote(dsend.at[to[0] * 8 + to[1]], dn.at[down_rows, down_cols], 3, to).start()
        return carry

    lax.fori_loop(1, HALF, send_rows(0), 0)

    scale = gain[...].reshape(1, 1, N)
    for i in range(LOADS):
        for j in range(3):
            load(i, j).wait()

        def round_one(e, carry):
            at = pl.ds(i * per + e * 2, 2)
            wsend[at, 0] = (g_stage[at] * scale).astype(bf16)
            wsend[at, 1] = (u_stage[at] * scale).astype(bf16)
            dsend[at] = d_stage[at].astype(bf16)
            return carry

        lax.fori_loop(0, per // 2, round_one, 0)

    lax.fori_loop(1, N, send_tiles, 0)
    lax.fori_loop(1, N, send_down, 0)
    lax.fori_loop(HALF, N, send_rows(1), 0)

    xrecv[0] = xsend[0]
    gu[:, my_rows, my_cols] = wsend[me]
    dn[down_rows, down_cols] = dsend[me]

    spread_t = jnp.where(iota((N, PAD * N), 1) // PAD == iota((N, PAD * N), 0), 1.0, 0.0)
    spread_t = spread_t.astype(bf16)
    weight_t = weight.T
    high = weight_t.astype(bf16)
    low = (weight_t - high.astype(f32)).astype(bf16)
    lanes = jnp.dot(rank.T.astype(bf16), spread_t, preferred_element_type=f32)
    hit = lanes == (iota((N, PAD * N), 1) % PAD).astype(f32)
    for i, part in enumerate((high, low)):
        wide = jnp.dot(part, spread_t, preferred_element_type=f32)
        mixw[i * N : (i + 1) * N, :] = jnp.where(hit, wide, 0.0).astype(bf16)

    other = (fs, tp + 1 - 2 * c)
    others = pl.ds(0, N - 1)
    early, late = pl.ds(0, HALF - 1), pl.ds(0, N - HALF)
    early_rows = remote(xsend.at[early, pl.ds(0, CAP)], xrecv.at[early, pl.ds(0, CAP)], 0, other)
    late_rows = remote(xsend.at[late, pl.ds(0, CAP)], xrecv.at[late, pl.ds(0, CAP)], 1, other)
    all_tiles = remote(wsend.at[others], wsend.at[others], 2, other)
    all_down = remote(dsend.at[others], dsend.at[others], 3, other)

    wide = (((1,), (1,)), ((), ()))

    def first(j, carry):
        block = xrecv[pl.ds(j * (ROWS // PAD), ROWS // PAD)].reshape(ROWS, D)
        gate_pre = lax.dot_general(block, gu[0], wide, preferred_element_type=f32)
        up_pre = lax.dot_general(block, gu[1], wide, preferred_element_type=f32)
        gate_part = jnp.minimum(gate_pre, clamp_limit)
        linear_part = jnp.clip(up_pre, -clamp_limit, clamp_limit)
        result = gate_part * jax.nn.sigmoid(sigmoid_slope * gate_part) * (linear_part + 1.0)
        act[pl.ds(pl.multiple_of(j * ROWS, ROWS), ROWS), :] = result.astype(bf16)
        return carry

    def back(k, carry):
        pltpu.make_async_remote_copy(
            src_ref=osend.at[k, pl.ds(0, CAP)], dst_ref=ret.at[k, pl.ds(0, CAP)],
            send_sem=send_sem.at[4], recv_sem=ret_sem.at[k // GROUP],
            device_id=behind(k), device_id_type=MESH,
        ).start()
        return carry

    def second(begin):
        def body(j, carry):
            part = act[pl.ds(pl.multiple_of(j * N, N), N), :]
            result = jnp.dot(part, dn[...], preferred_element_type=f32).astype(bf16)
            osend[pl.ds(j * GROUP, GROUP)] = result.reshape(GROUP, PAD, D)

            @pl.when(j > begin)
            def _():
                lax.fori_loop(lax.max((j - 1) * GROUP, 1), j * GROUP, back, 0)

            return carry

        return body

    early_rows.wait_recv()
    all_tiles.wait_recv()
    lax.fori_loop(0, PAD * HALF // ROWS, first, 0)
    all_down.wait_recv()
    lax.fori_loop(0, HALF // GROUP, second(0), 0)
    ret[0] = osend[0]
    lax.fori_loop(HALF - GROUP, HALF, back, 0)

    late_rows.wait_recv()
    lax.fori_loop(PAD * HALF // ROWS, PAD * N // ROWS, first, 0)
    lax.fori_loop(HALF // GROUP, N // GROUP, second(HALF // GROUP), 0)
    lax.fori_loop(N - GROUP, N, back, 0)

    for j, new in enumerate((gate_new, up_new)):
        def turn(b, carry):
            at = pl.ds(pl.multiple_of(b * 128, 128), 128)
            new[at, :] = gu[j, :, at].astype(f32).T.astype(bf16)
            return carry

        lax.fori_loop(0, D // 128, turn, 0)

    total[...] = jnp.zeros_like(total)
    for j in range(N // GROUP):
        count = GROUP - 1 if j == 0 else GROUP
        part = pl.ds(j * GROUP, count)
        pltpu.make_async_remote_copy(
            src_ref=osend.at[part, pl.ds(0, CAP)], dst_ref=ret.at[part, pl.ds(0, CAP)],
            send_sem=send_sem.at[4], recv_sem=ret_sem.at[j],
            device_id=other, device_id_type=MESH,
        ).wait_recv()
        block = ret[j * GROUP : (j + 1) * GROUP]
        block = jnp.where(iota(block.shape, 1) < CAP, block, jnp.zeros_like(block))
        both = jnp.dot(
            mixw[:, j * N : (j + 1) * N], block.reshape(N, D), preferred_element_type=f32
        )
        total[...] += both[:N] + both[N:]
    m_out[...] = total[...].astype(bf16)

    early_rows.wait_send()
    late_rows.wait_send()
    all_tiles.wait_send()
    all_down.wait_send()
    pltpu.make_async_remote_copy(
        src_ref=osend.at[others, pl.ds(0, CAP)], dst_ref=ret.at[others, pl.ds(0, CAP)],
        send_sem=send_sem.at[4], recv_sem=ret_sem.at[0], device_id=other, device_id_type=MESH,
    ).wait_send()


def write(*refs):
    sem = refs[8]
    copies = [pltpu.make_async_copy(refs[i], refs[4 + i], sem.at[i]) for i in range(4)]
    for copy in copies:
        copy.start()
    for copy in copies:
        copy.wait()


def shards(tokens, routes, route_weight, norm_gain, gate_weight, up_weight, down_weight):
    vmem = pl.BlockSpec(memory_space=pltpu.VMEM)
    anywhere = pl.BlockSpec(memory_space=pl.ANY)
    held = pl.pallas_call(
        kernel,
        out_shape=(
            pltpu.VMEM((D, FF), bf16),
            pltpu.VMEM((D, FF), bf16),
            pltpu.VMEM((FF, D), bf16),
            pltpu.VMEM((N, D), bf16),
        ),
        in_specs=[vmem, vmem, vmem, vmem, anywhere, anywhere, anywhere],
        out_specs=(vmem, vmem, vmem, vmem),
        scratch_shapes=[
            pltpu.VMEM((N, 64, 128), f32),
            pltpu.VMEM((N, 64, 128), f32),
            pltpu.VMEM((N, 32, 256), f32),
            pltpu.VMEM((N, 2, 64, 128), bf16),
            pltpu.VMEM((N, 32, 256), bf16),
            pltpu.VMEM((N, PAD, D), bf16),
            pltpu.VMEM((N, PAD, D), bf16),
            pltpu.VMEM((2, FF, D), bf16),
            pltpu.VMEM((N, PAD, D), bf16),
            pltpu.VMEM((N, PAD, D), bf16),
            pltpu.VMEM((PAD * N, FF), bf16),
            pltpu.VMEM((PAD * N, N), bf16),
            pltpu.VMEM((2 * N, PAD * N), bf16),
            pltpu.VMEM((N, D), bf16),
            pltpu.VMEM((N, D), f32),
            pltpu.SemaphoreType.DMA((3, LOADS)),
            pltpu.SemaphoreType.DMA((5,)),
            pltpu.SemaphoreType.DMA((4,)),
            pltpu.SemaphoreType.DMA((N // GROUP,)),
        ],
        compiler_params=pltpu.CompilerParams(
            collective_id=0, has_side_effects=True, vmem_limit_bytes=55 * 2**20
        ),
    )(
        tokens,
        routes.T,
        route_weight.T,
        norm_gain.reshape(1, N),
        jnp.swapaxes(gate_weight, 1, 2),
        jnp.swapaxes(up_weight, 1, 2),
        down_weight,
    )
    held = [pltpu.with_memory_space_constraint(array, pltpu.VMEM) for array in held]
    gate_new, up_new, down_new, mixed = pl.pallas_call(
        write,
        out_shape=[jax.ShapeDtypeStruct(array.shape, bf16) for array in held],
        in_specs=[vmem] * 4,
        out_specs=[anywhere] * 4,
        scratch_shapes=[pltpu.SemaphoreType.DMA((4,))],
        compiler_params=pltpu.CompilerParams(vmem_limit_bytes=2**20),
    )(*held)
    return gate_new[None], up_new[None], down_new[None], mixed


def solution(mesh):
    placed = (
        P(("fs", "tp"), None),
        P(("fs", "tp"), None),
        P(("fs", "tp"), None),
        P("fs"),
        P(None, "fs", "tp"),
        P(None, "fs", "tp"),
        P(None, "fs", "tp"),
    )
    return jax.shard_map(
        shards,
        mesh=mesh,
        in_specs=placed,
        out_specs=(
            P(("fs", "tp"), None, None),
            P(("fs", "tp"), None, None),
            P(("fs", "tp"), None, None),
            P(("fs", "tp"), None),
        ),
        check_vma=False,
    )
```

```python
import jax
import jax.numpy as jnp
from jax import lax
from jax.experimental import pallas as pl
from jax.experimental.pallas import tpu as pltpu
from jax.sharding import PartitionSpec as P

MESH = pl.DeviceIdType.MESH
f32, bf16 = jnp.float32, jnp.bfloat16

norm_epsilon = 1e-06
clamp_limit = 7.0
sigmoid_slope = 1.702

N = 128
D = 2048
FF = 512
CAP = 6
PAD = 8
STRIDE = 47
LOADS = 8
ROWS = 256
HALF = 64
GROUP = 16


def offset(k):
    kk = lax.rem(k * STRIDE, N)
    return kk // 32, lax.rem(kk // 8, 4), lax.rem(kk // 2, 4), lax.rem(kk, 2)


def kernel(
    tok, rt, rw, gain, g_in, u_in, d_in,
    gate_new, up_new, dn, m_out,
    g_stage, u_stage, d_stage, wsend, dsend, xsend, xrecv, gu, osend, ret,
    act, selb, mixw, normed, total,
    load_sem, send_sem, recv_sem, ret_sem,
):
    fs, tp = lax.axis_index("fs"), lax.axis_index("tp")
    z, y, x, c = fs // 4, lax.rem(fs, 4), tp // 2, lax.rem(tp, 2)
    me = fs * 8 + tp

    def ahead(k):
        dz, dy, dx, dc = offset(k)
        return (
            lax.rem(z + dz, 4) * 4 + lax.rem(y + dy, 4),
            lax.rem(x + dx, 4) * 2 + lax.rem(c + dc, 2),
        )

    def behind(k):
        dz, dy, dx, dc = offset(k)
        return (
            lax.rem(z + 4 - dz, 4) * 4 + lax.rem(y + 4 - dy, 4),
            lax.rem(x + 4 - dx, 4) * 2 + lax.rem(c + 2 - dc, 2),
        )

    barrier = pltpu.get_barrier_semaphore()

    def greet(k, carry):
        pl.semaphore_signal(barrier, inc=1, device_id=ahead(k), device_id_type=MESH)
        return carry

    lax.fori_loop(1, N, greet, 0)

    per = N // LOADS

    def load(i, j):
        src, dst = ((g_in, g_stage), (u_in, u_stage), (d_in, d_stage))[j]
        part = pl.ds(i * per, per)
        return pltpu.make_async_copy(src.at[part], dst.at[part], load_sem.at[j, i])

    for i in range(LOADS):
        for j in range(3):
            load(i, j).start()

    def iota(shape, dim):
        return lax.broadcasted_iota(jnp.int32, shape, dim)

    kk = (iota((N, N), 0) * STRIDE) & 127
    expert = (
        (((kk >> 5) + z) & 3) * 32
        + (((kk >> 3) + y) & 3) * 8
        + (((kk >> 1) + x) & 3) * 2
        + ((kk + c) & 1)
    )
    named = jnp.zeros((N, N), f32)
    weight = jnp.zeros((N, N), f32)
    for k in range(rt.shape[0]):
        hit = rt[k : k + 1, :] == expert
        named = jnp.where(hit, 1.0, named)
        weight = jnp.where(hit, rw[k : k + 1, :], weight)
    before = jnp.where(iota((N, N), 0) < iota((N, N), 1), 1.0, 0.0).astype(bf16)
    rank = jnp.dot(named.astype(bf16), before, preferred_element_type=f32)
    rank = jnp.where(named > 0.0, rank, -1.0)
    spread = jnp.where(iota((PAD * N, N), 0) // PAD == iota((PAD * N, N), 1), 1.0, 0.0)
    rows = jnp.dot(spread.astype(bf16), rank.astype(bf16), preferred_element_type=f32)
    place = (iota((PAD * N, N), 0) % PAD).astype(f32)
    selb[...] = jnp.where(rows == place, 1.0, 0.0).astype(bf16)

    values = tok[...].astype(f32)
    squares = jnp.mean(values * values, axis=1, keepdims=True)
    normed[...] = (values * lax.rsqrt(squares + norm_epsilon)).astype(bf16)

    def pick(i, carry):
        part = selb[pl.ds(pl.multiple_of(i * N, N), N), :]
        picked = jnp.dot(part, normed[...], preferred_element_type=f32).astype(bf16)
        xsend[pl.ds(i * GROUP, GROUP)] = picked.reshape(GROUP, PAD, D)
        return carry

    lax.fori_loop(0, N // GROUP, pick, 0)

    scale = gain[...].reshape(1, 1, N)
    for i in range(LOADS):
        for j in range(3):
            load(i, j).wait()

        def round_one(e, carry):
            at = pl.ds(i * per + e * 2, 2)
            wsend[at, 0] = (g_stage[at] * scale).astype(bf16)
            wsend[at, 1] = (u_stage[at] * scale).astype(bf16)
            dsend[at] = d_stage[at].astype(bf16)
            return carry

        lax.fori_loop(0, per // 2, round_one, 0)

    pl.semaphore_wait(barrier, N - 1)

    my_rows = pl.ds(pl.multiple_of(tp * 64, 64), 64)
    my_cols = pl.ds(pl.multiple_of(fs * 128, 128), 128)
    down_rows = pl.ds(pl.multiple_of(fs * 32, 32), 32)
    down_cols = pl.ds(pl.multiple_of(tp * 256, 256), 256)

    def remote(src, dst, i, to):
        return pltpu.make_async_remote_copy(
            src_ref=src, dst_ref=dst, send_sem=send_sem.at[i], recv_sem=recv_sem.at[i],
            device_id=to, device_id_type=MESH,
        )

    def send_rows(half):
        def send(k, carry):
            part = pl.ds(0, CAP)
            remote(xsend.at[k, part], xrecv.at[k, part], half, ahead(k)).start()
            return carry

        return send

    def send_tiles(k, carry):
        to = ahead(k)
        remote(wsend.at[to[0] * 8 + to[1]], gu.at[:, my_rows, my_cols], 2, to).start()
        return carry

    def send_down(k, carry):
        to = ahead(k)
        remote(dsend.at[to[0] * 8 + to[1]], dn.at[down_rows, down_cols], 3, to).start()
        return carry

    lax.fori_loop(1, HALF, send_rows(0), 0)

    lax.fori_loop(1, N, send_tiles, 0)
    lax.fori_loop(1, N, send_down, 0)
    lax.fori_loop(HALF, N, send_rows(1), 0)

    xrecv[0] = xsend[0]
    gu[:, my_rows, my_cols] = wsend[me]
    dn[down_rows, down_cols] = dsend[me]

    spread_t = jnp.where(iota((N, PAD * N), 1) // PAD == iota((N, PAD * N), 0), 1.0, 0.0)
    spread_t = spread_t.astype(bf16)
    weight_t = weight.T
    high = weight_t.astype(bf16)
    low = (weight_t - high.astype(f32)).astype(bf16)
    lanes = jnp.dot(rank.T.astype(bf16), spread_t, preferred_element_type=f32)
    hit = lanes == (iota((N, PAD * N), 1) % PAD).astype(f32)
    for i, part in enumerate((high, low)):
        wide = jnp.dot(part, spread_t, preferred_element_type=f32)
        mixw[i * N : (i + 1) * N, :] = jnp.where(hit, wide, 0.0).astype(bf16)

    other = (fs, tp + 1 - 2 * c)
    others = pl.ds(0, N - 1)
    early, late = pl.ds(0, HALF - 1), pl.ds(0, N - HALF)
    early_rows = remote(xsend.at[early, pl.ds(0, CAP)], xrecv.at[early, pl.ds(0, CAP)], 0, other)
    late_rows = remote(xsend.at[late, pl.ds(0, CAP)], xrecv.at[late, pl.ds(0, CAP)], 1, other)
    all_tiles = remote(wsend.at[others], wsend.at[others], 2, other)
    all_down = remote(dsend.at[others], dsend.at[others], 3, other)

    wide = (((1,), (1,)), ((), ()))

    def first(j, carry):
        block = xrecv[pl.ds(j * (ROWS // PAD), ROWS // PAD)].reshape(ROWS, D)
        gate_pre = lax.dot_general(block, gu[0], wide, preferred_element_type=f32)
        up_pre = lax.dot_general(block, gu[1], wide, preferred_element_type=f32)
        gate_part = jnp.minimum(gate_pre, clamp_limit)
        linear_part = jnp.clip(up_pre, -clamp_limit, clamp_limit)
        result = gate_part * jax.nn.sigmoid(sigmoid_slope * gate_part) * (linear_part + 1.0)
        act[pl.ds(pl.multiple_of(j * ROWS, ROWS), ROWS), :] = result.astype(bf16)
        return carry

    def back(k, carry):
        pltpu.make_async_remote_copy(
            src_ref=osend.at[k, pl.ds(0, CAP)], dst_ref=ret.at[k, pl.ds(0, CAP)],
            send_sem=send_sem.at[4], recv_sem=ret_sem.at[k // GROUP],
            device_id=behind(k), device_id_type=MESH,
        ).start()
        return carry

    def second(begin):
        def body(j, carry):
            part = act[pl.ds(pl.multiple_of(j * N, N), N), :]
            result = jnp.dot(part, dn[...], preferred_element_type=f32).astype(bf16)
            osend[pl.ds(j * GROUP, GROUP)] = result.reshape(GROUP, PAD, D)

            @pl.when(j > begin)
            def _():
                lax.fori_loop(lax.max((j - 1) * GROUP, 1), j * GROUP, back, 0)

            return carry

        return body

    early_rows.wait_recv()
    all_tiles.wait_recv()
    lax.fori_loop(0, PAD * HALF // ROWS, first, 0)
    all_down.wait_recv()
    lax.fori_loop(0, HALF // GROUP, second(0), 0)
    ret[0] = osend[0]
    lax.fori_loop(HALF - GROUP, HALF, back, 0)

    late_rows.wait_recv()
    lax.fori_loop(PAD * HALF // ROWS, PAD * N // ROWS, first, 0)
    lax.fori_loop(HALF // GROUP, N // GROUP, second(HALF // GROUP), 0)
    lax.fori_loop(N - GROUP, N, back, 0)

    for j, new in enumerate((gate_new, up_new)):
        def turn(b, carry):
            at = pl.ds(pl.multiple_of(b * 128, 128), 128)
            new[at, :] = gu[j, :, at].astype(f32).T.astype(bf16)
            return carry

        lax.fori_loop(0, D // 128, turn, 0)

    total[...] = jnp.zeros_like(total)
    for j in range(N // GROUP):
        count = GROUP - 1 if j == 0 else GROUP
        part = pl.ds(j * GROUP, count)
        pltpu.make_async_remote_copy(
            src_ref=osend.at[part, pl.ds(0, CAP)], dst_ref=ret.at[part, pl.ds(0, CAP)],
            send_sem=send_sem.at[4], recv_sem=ret_sem.at[j],
            device_id=other, device_id_type=MESH,
        ).wait_recv()
        block = ret[j * GROUP : (j + 1) * GROUP]
        block = jnp.where(iota(block.shape, 1) < CAP, block, jnp.zeros_like(block))
        both = jnp.dot(
            mixw[:, j * N : (j + 1) * N], block.reshape(N, D), preferred_element_type=f32
        )
        total[...] += both[:N] + both[N:]
    m_out[...] = total[...].astype(bf16)

    early_rows.wait_send()
    late_rows.wait_send()
    all_tiles.wait_send()
    all_down.wait_send()
    pltpu.make_async_remote_copy(
        src_ref=osend.at[others, pl.ds(0, CAP)], dst_ref=ret.at[others, pl.ds(0, CAP)],
        send_sem=send_sem.at[4], recv_sem=ret_sem.at[0], device_id=other, device_id_type=MESH,
    ).wait_send()


def write(*refs):
    sem = refs[8]
    copies = [pltpu.make_async_copy(refs[i], refs[4 + i], sem.at[i]) for i in range(4)]
    for copy in copies:
        copy.start()
    for copy in copies:
        copy.wait()


def shards(tokens, routes, route_weight, norm_gain, gate_weight, up_weight, down_weight):
    vmem = pl.BlockSpec(memory_space=pltpu.VMEM)
    anywhere = pl.BlockSpec(memory_space=pl.ANY)
    held = pl.pallas_call(
        kernel,
        out_shape=(
            pltpu.VMEM((D, FF), bf16),
            pltpu.VMEM((D, FF), bf16),
            pltpu.VMEM((FF, D), bf16),
            pltpu.VMEM((N, D), bf16),
        ),
        in_specs=[vmem, vmem, vmem, vmem, anywhere, anywhere, anywhere],
        out_specs=(vmem, vmem, vmem, vmem),
        scratch_shapes=[
            pltpu.VMEM((N, 64, 128), f32),
            pltpu.VMEM((N, 64, 128), f32),
            pltpu.VMEM((N, 32, 256), f32),
            pltpu.VMEM((N, 2, 64, 128), bf16),
            pltpu.VMEM((N, 32, 256), bf16),
            pltpu.VMEM((N, PAD, D), bf16),
            pltpu.VMEM((N, PAD, D), bf16),
            pltpu.VMEM((2, FF, D), bf16),
            pltpu.VMEM((N, PAD, D), bf16),
            pltpu.VMEM((N, PAD, D), bf16),
            pltpu.VMEM((PAD * N, FF), bf16),
            pltpu.VMEM((PAD * N, N), bf16),
            pltpu.VMEM((2 * N, PAD * N), bf16),
            pltpu.VMEM((N, D), bf16),
            pltpu.VMEM((N, D), f32),
            pltpu.SemaphoreType.DMA((3, LOADS)),
            pltpu.SemaphoreType.DMA((5,)),
            pltpu.SemaphoreType.DMA((4,)),
            pltpu.SemaphoreType.DMA((N // GROUP,)),
        ],
        compiler_params=pltpu.CompilerParams(
            collective_id=0, has_side_effects=True, vmem_limit_bytes=55 * 2**20
        ),
    )(
        tokens,
        routes.T,
        route_weight.T,
        norm_gain.reshape(1, N),
        jnp.swapaxes(gate_weight, 1, 2),
        jnp.swapaxes(up_weight, 1, 2),
        down_weight,
    )
    held = [pltpu.with_memory_space_constraint(array, pltpu.VMEM) for array in held]
    gate_new, up_new, down_new, mixed = pl.pallas_call(
        write,
        out_shape=[jax.ShapeDtypeStruct(array.shape, bf16) for array in held],
        in_specs=[vmem] * 4,
        out_specs=[anywhere] * 4,
        scratch_shapes=[pltpu.SemaphoreType.DMA((4,))],
        compiler_params=pltpu.CompilerParams(vmem_limit_bytes=2**20),
    )(*held)
    return gate_new[None], up_new[None], down_new[None], mixed


def solution(mesh):
    placed = (
        P(("fs", "tp"), None),
        P(("fs", "tp"), None),
        P(("fs", "tp"), None),
        P("fs"),
        P(None, "fs", "tp"),
        P(None, "fs", "tp"),
        P(None, "fs", "tp"),
    )
    return jax.shard_map(
        shards,
        mesh=mesh,
        in_specs=placed,
        out_specs=(
            P(("fs", "tp"), None, None),
            P(("fs", "tp"), None, None),
            P(("fs", "tp"), None, None),
            P(("fs", "tp"), None),
        ),
        check_vma=False,
    )
```
